32 devices in a mesh: sp: 8 (over z, x), tp: 4 (over y, core).
Axes of the slice: x: 2, y: 2, z: 4, core: 2. Of those that a mesh axis runs over, the one named last changes fastest.
Arguments:
- tokens: bfloat16 [2048, 1024], P(('sp', 'tp')), may hold values from -6 to 6
- doc_ids: int32 [2048], P('sp'), may hold values from 0 to 7, never falling along the last dimension, each value on 1 to 1536 neighbouring positions
- down_query: bfloat16 [1024, 256], P('sp'), may hold values from -0.1875 to 0.1875
- down_key: bfloat16 [1024, 256], P('sp'), may hold values from -0.1875 to 0.1875
- down_rotary: bfloat16 [1024, 32], P('sp'), may hold values from -0.1875 to 0.1875
- query_gain: float32 [256], replicated, may hold values from 0.1 to 1.9
- key_gain: float32 [256], replicated, may hold values from 0.1 to 1.9
- up_query: bfloat16 [256, 1536], P('sp', 'tp'), may hold values from -0.375 to 0.375
- up_key: bfloat16 [256, 1024], P('sp', 'tp'), may hold values from -0.375 to 0.375
- up_value: bfloat16 [256, 1024], P('sp', 'tp'), may hold values from -0.375 to 0.375
- output_weight: bfloat16 [1024, 1024], P('tp', 'sp'), may hold values from -0.1875 to 0.1875
- out_gain: float32 [1024], replicated, may hold values from 0.1 to 1.9
Outputs:
- mixed: bfloat16 [2048, 1024], P(('sp', 'tp'))
- log_sums: float32 [2048, 16], P('sp', 'tp')
The draws below stay inside these ranges and needn't reach their ends.
Inputs may be any that keep to these rules, and one draw needn't show every extreme that they name: doc_ids never fall along the sequence and run from 0 to at most the number of devices along sp minus one; each document has 1 to 1536 positions, and one document has exactly that many.
All inputs are finite; a program needn't handle non-finite values.
Results may differ from the reference program's by a relative error of at most 0.02.
Values may be sent and summed in bfloat16 or wider, within the bound.
A program may use at most 64 MiB of HBM per device.

```python
import math
import jax
import jax.numpy as jnp
import numpy as np
from jax import lax

D = 1024
HEADS = 16
Q_RANK = 256
KV_RANK = 256
NOPE = 64
ROPE = 32
VDIM = 64
TOK_DEV = 256
TOKENS = 2048
N_SP = 8


def block_scale(key, extent, pieces, least, high):
    def one(position, shards_of):
        draws = jax.random.uniform(jax.random.fold_in(jax.random.fold_in(key, 6), position), (shards_of,), jnp.float32, least / len(pieces), high / len(pieces))
        return jnp.repeat(jnp.exp(draws), extent[position] // shards_of).reshape((-1,) + (1,) * (len(extent) - position - 1))

    level = one(*pieces[0])
    for cut in pieces[1:]:
        level = level * one(*cut)
    return level


def profile(number_of, total, bound, skew):
    portions = [(1 << 20) // math.isqrt(standing ** skew) + 1 for standing in range(2, number_of + 1)]
    rest, given = total - bound - (number_of - 1), [1] * (number_of - 1)
    while rest > 0:
        movable = [i for i in range(number_of - 1) if given[i] < bound]
        pool, budget = sum([portions[i] for i in movable]), rest
        for i in movable:
            more = min(bound - given[i], max(1, budget * portions[i] // pool), rest)
            given[i] = given[i] + more
            rest = rest - more
    return np.array([bound] + given)


def uneven_parts(key, count, total, bound, lean):
    if count == 2:
        one = jax.random.randint(key, (), max(1, total - bound), min(bound, total - 1) + 1)
        return jnp.stack([one, total - one])
    lengths = jnp.asarray(profile(count, total, bound, lean), jnp.int32)
    twos = (count - 1) // 2
    source_of, sink = lengths[1:1 + 2 * twos:2], lengths[2:2 + 2 * twos:2]
    room = jnp.minimum(source_of - 1, bound - sink)
    moved = jax.random.randint(jax.random.fold_in(key, 1), (twos,), 0, 1 << 20) % (room + 1)
    lengths = lengths.at[1:1 + 2 * twos:2].set(source_of - moved).at[2:2 + 2 * twos:2].set(sink + moved)
    return lengths[jax.random.permutation(jax.random.fold_in(key, 2), count)]


def normal_values(own_key, shape, width, bound, split=(), kind=jnp.bfloat16):
    values = width * jax.random.normal(own_key, shape, jnp.float32)
    if split:
        values = values * block_scale(own_key, shape, split, -0.22, 0.18)
    return jnp.clip(values, -bound, bound).astype(kind)


def setup_inputs(seed: int = 0) -> dict:
    seeds = jax.random.split(jax.random.key(seed), 13)
    return {
        "tokens": normal_values(seeds[0], (TOKENS, D), 1.0, 6.0, ((0, 32),)),
        "doc_ids": jnp.searchsorted(jnp.cumsum(uneven_parts(seeds[1], N_SP, TOKENS, TOK_DEV * N_SP // 2 + 2 * TOK_DEV, 2)), jnp.arange(TOKENS), side="right").astype(jnp.int32),
        "down_query": normal_values(seeds[2], (D, Q_RANK), D ** -0.5, 0.1875, ((0, 8),)),
        "down_key": normal_values(seeds[3], (D, KV_RANK), D ** -0.5, 0.1875, ((0, 8),)),
        "down_rotary": normal_values(seeds[4], (D, ROPE), D ** -0.5, 0.1875, ((0, 8),)),
        "query_gain": jnp.clip(1.0 + 0.18 * jax.random.normal(seeds[5], (Q_RANK,), jnp.float32), 0.1, 1.9),
        "key_gain": jnp.clip(1.0 + 0.18 * jax.random.normal(seeds[6], (KV_RANK,), jnp.float32), 0.1, 1.9),
        "up_query": normal_values(seeds[7], (Q_RANK, HEADS * (NOPE + ROPE)), Q_RANK ** -0.5, 0.375, ((0, 8), (1, 4))),
        "up_key": normal_values(seeds[8], (KV_RANK, HEADS * NOPE), KV_RANK ** -0.5, 0.375, ((0, 8), (1, 4))),
        "up_value": normal_values(seeds[9], (KV_RANK, HEADS * VDIM), KV_RANK ** -0.5, 0.375, ((0, 8), (1, 4))),
        "output_weight": normal_values(seeds[10], (HEADS * VDIM, D), (HEADS * VDIM) ** -0.5, 0.1875, ((0, 4), (1, 8))),
        "out_gain": jnp.clip(1.0 + 0.18 * jax.random.normal(seeds[11], (D,), jnp.float32), 0.1, 1.9),
    }


NEG_BIG = -1e+30
THETA = 10000.0
EPS = 1e-06

def settle(quantity):
    return lax.optimization_barrier(quantity.astype(jnp.bfloat16))

def rms_gain(summed, gain_vector):
    widened = settle(summed).astype(jnp.float32)
    scaled = widened * lax.rsqrt(lax.optimization_barrier(jnp.mean(widened * widened, axis=-1, keepdims=True)) + EPS)
    return (scaled * gain_vector).astype(jnp.bfloat16)

def rotate(vectors, positions):
    half_width = vectors.shape[-1] // 2
    inverse = THETA ** (-jnp.arange(half_width, dtype=jnp.float32) / half_width)
    angles = positions.astype(jnp.float32)[:, None] * inverse[None, :]
    angles = angles.reshape((vectors.shape[0],) + (1,) * (vectors.ndim - 2) + (half_width,))
    cosine_part = jnp.cos(angles)
    sine_part = jnp.sin(angles)
    widened = vectors.astype(jnp.float32)
    front_half = widened[..., :half_width]
    back_half = widened[..., half_width:]
    return jnp.concatenate([front_half * cosine_part - back_half * sine_part, back_half * cosine_part + front_half * sine_part], axis=-1).astype(jnp.bfloat16)

def reference(tokens, doc_ids, down_query, down_key, down_rotary, query_gain, key_gain, up_query, up_key, up_value, output_weight, out_gain):
    highest = lax.Precision.HIGHEST
    positions = jnp.arange(TOKENS, dtype=jnp.int32)
    query_latent = rms_gain(jnp.dot(tokens, down_query, preferred_element_type=jnp.float32), query_gain)
    key_latent = rms_gain(jnp.dot(tokens, down_key, preferred_element_type=jnp.float32), key_gain)
    key_turned = rotate(settle(jnp.dot(tokens, down_rotary, preferred_element_type=jnp.float32)), positions)
    queries = settle(jnp.dot(query_latent, up_query, preferred_element_type=jnp.float32))
    queries = queries.reshape(TOKENS, HEADS, NOPE + ROPE)
    query_plain = queries[..., :NOPE]
    query_turned = rotate(queries[..., NOPE:], positions)
    key_plain = settle(jnp.dot(key_latent, up_key, preferred_element_type=jnp.float32)).reshape(TOKENS, HEADS, NOPE)
    values = settle(jnp.dot(key_latent, up_value, preferred_element_type=jnp.float32)).reshape(TOKENS, HEADS, VDIM)
    score_scale = 1.0 / math.sqrt(NOPE + ROPE)
    plain_wide = key_plain.astype(jnp.float32)
    turned_wide = key_turned.astype(jnp.float32)
    values_wide = values.astype(jnp.float32)

    def one_block(block_parts):
        plain_block, turned_block, docs_block = block_parts
        scores = jnp.einsum('qhd,khd->hqk', plain_block.astype(jnp.float32), plain_wide, precision=highest)
        scores = scores + jnp.einsum('qhr,kr->hqk', turned_block.astype(jnp.float32), turned_wide, precision=highest)
        scores = scores * score_scale
        same_doc = (docs_block[:, None] == doc_ids[None, :])[None]
        top_score = lax.optimization_barrier(jnp.max(jnp.where(same_doc, scores, NEG_BIG), axis=-1, keepdims=True))
        weights = jnp.where(same_doc, jnp.exp(scores - top_score), 0.0)
        weight_sum = lax.optimization_barrier(jnp.sum(weights, axis=-1))
        mixed_rows = jnp.einsum('hqk,khv->qhv', settle(weights).astype(jnp.float32), values_wide, precision=highest)
        mixed_rows = mixed_rows / weight_sum.T[:, :, None]
        return (mixed_rows, (top_score[..., 0] + jnp.log(weight_sum)).T)
    blocks = (query_plain.reshape(N_SP, TOK_DEV, HEADS, NOPE), query_turned.reshape(N_SP, TOK_DEV, HEADS, ROPE), doc_ids.reshape(N_SP, TOK_DEV))
    mixed_rows, log_sums = lax.map(one_block, blocks)
    attended = mixed_rows.reshape(TOKENS, HEADS * VDIM).astype(jnp.bfloat16)
    log_sums = log_sums.reshape(TOKENS, HEADS)
    projected = jnp.dot(attended, output_weight, preferred_element_type=jnp.float32)
    return (rms_gain(projected, out_gain), log_sums)
```

```python
import functools
import math

import jax
import jax.numpy as jnp
import numpy as np
from jax import lax
from jax.experimental import pallas as pl
from jax.experimental.pallas import tpu as pltpu
from jax.sharding import PartitionSpec as P

NOPE = 64
ROPE = 32
VDIM = 64
THETA = 10000.0
EPS = 1e-06
MASKED = -1e30
MESH = pl.DeviceIdType.MESH
F32 = jnp.float32
BF16 = jnp.bfloat16


def dot(a, b):
    return jnp.dot(a, b, preferred_element_type=F32)


def rows_joined(blocks, flat):
    n, r, c = blocks.shape
    for j in range(n):
        flat[j * r : (j + 1) * r, :] = blocks[j]
    return flat


def rms_parts(parts, gains):
    wide = [part.astype(F32) for part in parts]
    width = sum(part.shape[-1] for part in parts)
    total = sum(jnp.sum(part * part, axis=-1, keepdims=True) for part in wide)
    scale = lax.rsqrt(total / width + EPS)
    return [(part * scale * gain).astype(BF16) for part, gain in zip(wide, gains)]


def tables(tokens, heads):
    half = ROPE // 2
    inverse = np.float32(THETA) ** (-np.arange(half, dtype=np.float32) / np.float32(half))
    angles = np.arange(tokens, dtype=np.float32)[:, None] * inverse.astype(np.float32)[None, :]
    turn = np.zeros((tokens, 256), np.float32)
    turn[:, :ROPE] = np.tile(np.cos(angles), (1, 2))
    turn[:, 128 : 128 + ROPE] = np.tile(np.sin(angles), (1, 2))
    width = NOPE + ROPE
    pick = np.zeros((heads * width, heads * 384), np.float32)
    eye = np.arange(NOPE)
    rot = np.arange(ROPE)
    for head in range(heads):
        pick[head * width + eye, head * 384 + (head % 2) * NOPE + eye] = 1
        pick[head * width + NOPE + rot, head * 384 + 128 + rot] = 1
        low = np.arange(half)
        pick[head * width + NOPE + half + low, head * 384 + 256 + low] = -1
        pick[head * width + NOPE + low, head * 384 + 256 + half + low] = 1
    pick_key = np.zeros((ROPE, 256), np.float32)
    pick_key[rot, rot] = 1
    pick_key[half + low, 128 + low] = -1
    pick_key[low, 128 + half + low] = 1
    return turn, pick, pick_key


def kernel(
    n, ntp, heads,
    tokens, docs, down_q, down_k, down_r, gain_q, gain_k, up_q, up_k, up_v, out_w, gain_o,
    turn, pick, pick_key,
    out, log_out,
    tok, wd, wr, uq, up, wo, qraw, kraw, krot, tab, sel, qs, values, scores, att, part, got_core, got_y, send_y, wd_flat, wr_flat, uq_flat, up_flat,
    loc, s_uq, r_uq, s_tok, r_tok, s_wd, r_wd, s_wr, r_wr, s_up, r_up, s_wo, r_wo,
    s_q, r_q, s_k, r_k, s_ky, r_ky, s_kc, r_kc, s_kr, r_kr, s_krc, r_krc, s_f, r_f,
):
    half = n // 2
    me = lax.axis_index("sp")
    t = lax.axis_index("tp")
    ny = ntp // 2
    y = t // 2
    yh = lax.rem(y, 2)
    core = lax.rem(t, 2)
    own = tokens.shape[0]
    block = ntp * own
    side = block // 2
    cols = wd.shape[-1]
    partner = me + 1 - 2 * lax.rem(me, 2)
    other_core = t + 1 - 2 * core
    other_y = (y + 1 - 2 * yh) * 2 + core

    def dev(sp, tp):
        return (sp, tp)

    x_dev = dev(partner, t)
    y_dev = dev(me, other_y)
    c_dev = dev(me, other_core)

    col = pl.multiple_of(yh * cols, cols)
    c_tok = pltpu.make_async_copy(tokens, tok.at[t], loc.at[0])
    c_wr = pltpu.make_async_copy(down_r, wr.at[me], loc.at[2])
    nq, nk = up_q.shape[1], up_k.shape[1]
    c_up = [
        pltpu.make_async_copy(up_q, uq.at[me], loc.at[3]),
        pltpu.make_async_copy(up_k, up.at[me, :, pl.ds(0, nk)], loc.at[4]),
        pltpu.make_async_copy(up_v, up.at[me, :, pl.ds(nk, nk)], loc.at[5]),
    ]
    c_wo = pltpu.make_async_copy(out_w, wo.at[me], loc.at[6])
    c_tab = pltpu.make_async_copy(turn.at[me], tab, loc.at[7])
    c_sel = pltpu.make_async_copy(pick, sel, loc.at[8])
    c_tok.start()

    @pl.when(core == 0)
    def _():
        pltpu.make_async_copy(down_k.at[:, pl.ds(col, cols)], wd.at[me], loc.at[1]).start()

    @pl.when(core == 1)
    def _():
        pltpu.make_async_copy(down_q.at[:, pl.ds(col, cols)], wd.at[me], loc.at[1]).start()

    c_wd = pltpu.make_async_copy(down_q.at[:, pl.ds(0, cols)], wd.at[me], loc.at[1])
    for copy in [c_wr] + c_up + [c_wo, c_tab, c_sel]:
        copy.start()

    barrier = pltpu.get_barrier_semaphore()
    for k in range(1, n):
        pl.semaphore_signal(barrier, inc=1, device_id=dev(lax.rem(me + k, n), t), device_id_type=MESH)
    for k in range(1, ntp):
        pl.semaphore_signal(barrier, inc=1, device_id=dev(me, lax.rem(t + k, ntp)), device_id_type=MESH)

    def rc(src, dst, s, r, device):
        return pltpu.make_async_remote_copy(
            src_ref=src, dst_ref=dst, send_sem=s, recv_sem=r, device_id=device, device_id_type=MESH
        )

    class Gather:
        def __init__(self, at, s, r):
            self.at, self.s, self.r = at, s, r

        def z(self, k):
            return rc(self.at(me), self.at(me), self.s.at[k], self.r.at[k], dev(lax.rem(me + 2 * k, n), t))

        def x(self, k):
            ref = self.at(lax.rem(me - 2 * k + n, n))
            return rc(ref, ref, self.s.at[half + k], self.r.at[half + k], x_dev)

        def start_z(self):
            for k in range(1, half):
                self.z(k).start()

        def from_z(self, k):
            ref = self.at(lax.rem(me - 2 * k + n, n))
            rc(ref, ref, self.s.at[k], self.r.at[k], x_dev).wait_recv()

        def from_x(self, k):
            ref = self.at(lax.rem(partner - 2 * k + n, n))
            rc(ref, ref, self.s.at[half + k], self.r.at[half + k], x_dev).wait_recv()

        def hand_on(self):
            for k in range(1, half):
                self.from_z(k)
                self.x(k).start()

        def rest(self):
            for k in range(half):
                self.from_x(k)

        def drain(self):
            for k in range(1, half):
                self.z(k).wait_send()
            for k in range(half):
                self.x(k).wait_send()

    g_wd = Gather(lambda i: wd.at[i], s_wd, r_wd)
    g_wr = Gather(lambda i: wr.at[i], s_wr, r_wr)
    g_uq = Gather(lambda i: uq.at[i], s_uq, r_uq)
    g_up = Gather(lambda i: up.at[i], s_up, r_up)
    g_wo = Gather(lambda i: wo.at[i], s_wo, r_wo)
    g_k = Gather(lambda i: kraw.at[i, yh], s_k, r_k)
    g_kr = Gather(lambda i: krot.at[i], s_kr, r_kr)

    c_wd.wait()
    c_wr.wait()
    c_tok.wait()
    pl.semaphore_wait(barrier, n - 1 + ntp - 1)

    def y_at(k):
        return lax.rem(y + k, ny) * 2 + core

    def tok_y(k):
        return rc(tok.at[t], tok.at[t], s_tok.at[k], r_tok.at[k], dev(me, y_at(k)))

    def tok_from(k):
        ref = tok.at[y_at(ny - k)]
        return rc(ref, ref, s_tok.at[k], r_tok.at[k], c_dev)

    def tok_c(k):
        ref = tok.at[y_at(ny - k)]
        return rc(ref, ref, s_tok.at[ny + k], r_tok.at[ny + k], c_dev)

    for k in range(1, ny):
        tok_y(k).start()
    g_wd.start_z()
    g_wd.x(0).start()

    @pl.when(core == 1)
    def _():
        g_wr.start_z()
        g_wr.x(0).start()

    tok_c(0).start()
    for copy in c_up:
        copy.wait()
    g_up.start_z()
    g_uq.start_z()
    g_wd.hand_on()

    @pl.when(core == 1)
    def _():
        g_wr.hand_on()

    g_up.x(0).start()
    g_uq.x(0).start()
    for k in range(1, ny):
        tok_from(k).wait_recv()
        tok_c(k).start()

    down = lax.broadcasted_iota(jnp.int32, (block, block), 0)
    across = lax.broadcasted_iota(jnp.int32, (block, block), 1)
    doc_row = jnp.broadcast_to(docs[...].astype(F32), (block, block))
    doc_col = jnp.sum(jnp.where(down == across, doc_row, 0.0), axis=-1, keepdims=True)
    lane = lax.broadcasted_iota(jnp.int32, (block, 128), 1)
    in_docs = (lane >= ROPE) & (lane < ROPE + n)
    same = doc_col == (lane - ROPE).astype(F32)
    key_docs = jnp.where(in_docs & same, 1.0, 0.0)
    query_docs = jnp.where(in_docs & jnp.logical_not(same), MASKED, 0.0)

    for k in range(ny):
        tok_c(k).wait_recv()
    g_wd.rest()
    block_tokens = tok[...].reshape(block, tok.shape[-1])
    raw = dot(block_tokens, rows_joined(wd, wd_flat)[...]).astype(BF16)
    c_tab.wait()

    q_y = rc(qraw.at[yh], qraw.at[yh], s_q.at[0], r_q.at[0], y_dev)
    q_c = rc(qraw.at[yh], qraw.at[yh], s_q.at[1], r_q.at[1], c_dev)
    q_f = rc(qraw.at[1 - yh], qraw.at[1 - yh], s_q.at[2], r_q.at[2], c_dev)

    def k_y(i, slot):
        return rc(kraw.at[i, yh], kraw.at[i, yh], s_ky.at[slot], r_ky.at[slot], y_dev)

    def k_from_y(i, slot):
        return rc(kraw.at[i, 1 - yh], kraw.at[i, 1 - yh], s_ky.at[slot], r_ky.at[slot], y_dev)

    def k_c(i, which, slot):
        ref = kraw.at[i, which]
        return rc(ref, ref, s_kc.at[slot], r_kc.at[slot], c_dev)

    def kr_c(i, slot):
        return rc(krot.at[i], krot.at[i], s_krc.at[slot], r_krc.at[slot], c_dev)

    def block_of(slot):
        if slot < half:
            return lax.rem(me - 2 * slot + n, n)
        return lax.rem(partner - 2 * (slot - half) + n, n)

    @pl.when(core == 0)
    def _():
        kraw[me, yh] = raw
        g_k.start_z()
        g_k.x(0).start()
        k_y(me, 0).start()
        k_c(me, yh, 0).start()

    @pl.when(core == 1)
    def _():
        qraw[yh] = raw
        q_y.start()
        q_c.start()
        g_wr.rest()
        rotary = dot(block_tokens, rows_joined(wr, wr_flat)[...]).astype(BF16)
        both = dot(rotary, pick_key[...])
        turned = both[:, :128] * tab[:, :128] + both[:, 128:] * tab[:, 128:] + key_docs
        packed = turned[:side] + pltpu.roll(turned[side:], 64, 1)
        krot[me] = packed.astype(BF16)
        g_kr.start_z()
        g_kr.x(0).start()
        kr_c(me, 0).start()
        q_y.wait_recv()
        q_f.start()

    g_up.hand_on()
    g_uq.hand_on()
    c_wo.wait()

    g_wo.start_z()

    @pl.when(core == 0)
    def _():
        for k in range(1, half):
            g_k.from_z(k)
            g_k.x(k).start()
            k_y(block_of(k), k).start()
            k_c(block_of(k), yh, k).start()

    @pl.when(core == 1)
    def _():
        for k in range(1, half):
            g_kr.from_z(k)
            g_kr.x(k).start()
            kr_c(block_of(k), k).start()

    g_wo.x(0).start()
    g_up.rest()
    g_uq.rest()

    @pl.when(core == 0)
    def _():
        q_c.wait_recv()
        q_f.wait_recv()

    c_sel.wait()
    gq = gain_q[...]
    lat = rms_parts([qraw[0], qraw[1]], [gq[:, :cols], gq[:, cols:]])
    rows_joined(up, up_flat)
    rows_joined(uq, uq_flat)
    projected = (dot(lat[0], uq_flat[:cols, :]) + dot(lat[1], uq_flat[cols:, :])).astype(BF16)
    for head in range(heads):
        laid = dot(projected, sel[:, head * 384 : (head + 1) * 384])
        turned = laid[:, 128:256] * tab[:, :128] + laid[:, 256:] * tab[:, 128:] + query_docs
        plain = laid[:, :128].astype(BF16)
        rows = pl.ds((head % 2) * block, block)
        qs[head // 2, 0, rows, :128] = plain
        qs[head // 2, 1, rows, :128] = plain
        qs[head // 2, 0, rows, 128:] = turned.astype(BF16)
        qs[head // 2, 1, rows, 128:] = pltpu.roll(turned, 64, 1).astype(BF16)

    gk = gain_k[...]
    for slot in range(n):
        i = block_of(slot)

        @pl.when(core == 0)
        def _(slot=slot, i=i):
            if slot >= half:
                g_k.from_x(slot - half)
                k_y(i, slot).start()
                k_c(i, yh, slot).start()
            k_from_y(i, slot).wait_recv()
            k_c(i, 1 - yh, n + slot).start()
            kr_c(i, slot).wait_recv()

        @pl.when(core == 1)
        def _(slot=slot, i=i):
            if slot >= half:
                g_kr.from_x(slot - half)
                kr_c(i, slot).start()
            k_c(i, yh, slot).wait_recv()
            k_c(i, 1 - yh, n + slot).wait_recv()

        if slot > 0 and slot < half:
            g_wo.from_z(slot)
            g_wo.x(slot).start()

        lat = rms_parts([kraw[i, 0], kraw[i, 1]], [gk[:, :cols], gk[:, cols:]])
        kv = (dot(lat[0], up_flat[:cols, :]) + dot(lat[1], up_flat[cols:, :])).astype(BF16)
        values[i] = kv[:, nk:]
        rot = krot[i]
        for pair in range(heads // 2):
            for s in range(2):
                keys = jnp.concatenate(
                    [kv[s * side : (s + 1) * side, pair * 128 : (pair + 1) * 128], rot], axis=1
                )
                scores[pair, i, :, s * side : (s + 1) * side] = lax.dot_general(
                    qs[pair, s], keys, (((1,), (1,)), ((), ())), preferred_element_type=F32
                )

    scale = 1.0 / math.sqrt(NOPE + ROPE)
    factor = scale * math.log2(math.e)
    head_lane = lax.broadcasted_iota(jnp.int32, (block, nk), 1) // VDIM
    attended = jnp.zeros((block, nk), F32)
    sums = []
    for head in range(heads):
        rows = pl.ds((head % 2) * block, block)
        top = scores[head // 2, 0, rows, :]
        for i in range(1, n):
            top = jnp.maximum(top, scores[head // 2, i, rows, :])
        top = jnp.max(top, axis=-1, keepdims=True)
        shift = top * factor
        total = jnp.zeros((block, block), F32)
        mixed = jnp.zeros((block, nk), F32)
        for i in range(n):
            weights = jnp.exp2(scores[head // 2, i, rows, :] * factor - shift)
            total = total + weights
            mixed = mixed + dot(weights.astype(BF16), values[i])
        weight_sum = jnp.sum(total, axis=-1, keepdims=True)
        attended = jnp.where(head_lane == head, mixed / weight_sum, attended)
        sums.append(top * scale + jnp.log(weight_sum))
    log_out[...] = jnp.concatenate(sums, axis=1)
    att[...] = attended.astype(BF16)

    g_wo.rest()

    def partial(owner):
        rows = att[pl.ds(pl.multiple_of(owner * own, own), own), :]
        return jnp.concatenate([dot(rows, wo[j]) for j in range(n)], axis=1)

    def f_c(k):
        return rc(part.at[k], got_core.at[k], s_f.at[k], r_f.at[k], c_dev)

    def f_y(k):
        return rc(send_y.at[k], got_y.at[k], s_f.at[ny + k], r_f.at[ny + k], dev(me, y_at(k)))

    order = list(range(1, ny)) + [0]
    for k in order:
        part[k] = partial(lax.rem(y + k, ny) * 2 + 1 - core).astype(BF16)
        f_c(k).start()
    for k in order[:-1]:
        far = partial(y_at(k))
        f_c(k).wait_recv()
        send_y[k] = (far + got_core[k].astype(F32)).astype(BF16)
        f_y(k).start()
    near = partial(t)
    f_c(0).wait_recv()
    near = near + got_core[0].astype(F32)
    for k in order[:-1]:
        f_y(k).wait_recv()
        near = near + got_y[k].astype(F32)
    out[...] = rms_parts([near.astype(BF16)], [gain_o[...]])[0]

    for k in range(ny):
        tok_c(k).wait_send()
        f_c(k).wait_send()
        if k > 0:
            tok_y(k).wait_send()
            f_y(k).wait_send()
    for gather in (g_wd, g_up, g_uq, g_wo):
        gather.drain()

    @pl.when(core == 0)
    def _():
        g_k.drain()
        for slot in range(n):
            k_y(block_of(slot), slot).wait_send()
            k_c(block_of(slot), yh, slot).wait_send()
            k_c(block_of(slot), 1 - yh, n + slot).wait_send()

    @pl.when(core == 1)
    def _():
        g_wr.drain()
        g_kr.drain()
        for slot in range(n):
            kr_c(block_of(slot), slot).wait_send()
        for copy in (q_y, q_c, q_f):
            copy.wait_send()


def on_device(n, ntp, tokens, doc_ids, down_q, down_k, down_r, gain_q, gain_k, up_q, up_k, up_v, out_w, gain_o):
    own, width = tokens.shape
    block = doc_ids.shape[0]
    heads = up_k.shape[1] // NOPE
    rank = down_k.shape[1]
    cols = rank // 2
    nq, nk, nv = up_q.shape[1], up_k.shape[1], up_v.shape[1]
    turn, pick, pick_key = tables(n * block, heads)
    turn = jnp.asarray(turn.reshape(n, block, 256))
    vmem = pl.BlockSpec(memory_space=pltpu.VMEM)
    hbm = pl.BlockSpec(memory_space=pl.ANY)
    dma = lambda k: pltpu.SemaphoreType.DMA((k,))
    scratch = [
        pltpu.VMEM((ntp, own, width), BF16),
        pltpu.VMEM((n, width // n, cols), BF16),
        pltpu.VMEM((n, width // n, down_r.shape[1]), BF16),
        pltpu.VMEM((n, up_q.shape[0], nq), BF16),
        pltpu.VMEM((n, up_q.shape[0], nk + nv), BF16),
        pltpu.VMEM((n,) + out_w.shape, BF16),
        pltpu.VMEM((2, block, cols), BF16),
        pltpu.VMEM((n, 2, block, cols), BF16),
        pltpu.VMEM((n, block // 2, 128), BF16),
        pltpu.VMEM((block, 256), F32),
        pltpu.VMEM(pick.shape, BF16),
        pltpu.VMEM((heads // 2, 2, 2 * block, 256), BF16),
        pltpu.VMEM((n, block, nv), BF16),
        pltpu.VMEM((heads // 2, n, 2 * block, block), F32),
        pltpu.VMEM((block, nv), BF16),
        pltpu.VMEM((ntp // 2, own, width), BF16),
        pltpu.VMEM((ntp // 2, own, width), BF16),
        pltpu.VMEM((ntp // 2, own, width), BF16),
        pltpu.VMEM((ntp // 2, own, width), BF16),
        pltpu.VMEM((width, cols), BF16),
        pltpu.VMEM((width, down_r.shape[1]), BF16),
        pltpu.VMEM((rank, nq), BF16),
        pltpu.VMEM((rank, nk + nv), BF16),
        dma(9), dma(n), dma(n), dma(ntp), dma(ntp),
        dma(n), dma(n), dma(n), dma(n), dma(n), dma(n), dma(n), dma(n),
        dma(3), dma(3), dma(n), dma(n), dma(n), dma(n),
        dma(2 * n), dma(2 * n), dma(n), dma(n), dma(n), dma(n), dma(ntp), dma(ntp),
    ]
    return pl.pallas_call(
        functools.partial(kernel, n, ntp, heads),
        out_shape=(
            jax.ShapeDtypeStruct((own, width), BF16),
            jax.ShapeDtypeStruct((block, heads), F32),
        ),
        in_specs=[hbm, vmem, hbm, hbm, hbm, vmem, vmem, hbm, hbm, hbm, hbm, vmem, hbm, hbm, vmem],
        out_specs=(vmem, vmem),
        scratch_shapes=scratch,
        compiler_params=pltpu.CompilerParams(
            collective_id=0, has_side_effects=True, vmem_limit_bytes=60 * 1024 * 1024
        ),
    )(
        tokens, doc_ids[None, :], down_q, down_k, down_r, gain_q[None, :], gain_k[None, :],
        up_q, up_k, up_v, out_w, gain_o[None, :],
        turn, jnp.asarray(pick, BF16), jnp.asarray(pick_key, BF16),
    )


def solution(mesh):
    assert mesh.shape["tp"] % 4 == 0 and mesh.shape["sp"] % 2 == 0 and mesh.shape["sp"] <= 32
    placed = (
        P(("sp", "tp"), None), P("sp"), P("sp", None), P("sp", None), P("sp", None), P(), P(),
        P("sp", "tp"), P("sp", "tp"), P("sp", "tp"), P("tp", "sp"), P(),
    )
    return jax.shard_map(
        functools.partial(on_device, mesh.shape["sp"], mesh.shape["tp"]),
        mesh=mesh,
        in_specs=placed,
        out_specs=(P(("sp", "tp"), None), P("sp", "tp")),
        check_vma=False,
    )
```
